512 devices in a mesh: gr: 2 (over z_hi), fs: 32 (over z_lo, y), tp: 8 (over x, core).
Axes of the slice: x: 4, y: 4, z: 16 (z_hi: 2, z_lo: 8; z = z_hi * 8 + z_lo), core: 2. Of those that a mesh axis runs over, the one named last changes fastest.
Arguments:
- tokens: bfloat16 [8192, 2048], P(('gr', 'fs')), may hold values from -6 to 6
- norm_gain: float32 [2048], P(('gr', 'fs')), may hold values from 0.1 to 1.9
- gate_train: float32 [32, 2048, 1024], P(None, ('gr', 'fs'), 'tp'), may hold values from -0.3125 to 0.3125
- up_train: float32 [32, 2048, 1024], P(None, ('gr', 'fs'), 'tp'), may hold values from -0.3125 to 0.3125
- down_train: float32 [32, 1024, 2048], P(None, ('gr', 'fs'), 'tp'), may hold values from -0.09375 to 0.09375
- routes: int32 [8192, 4], P(('gr', 'fs')), may hold values from 0 to 31, all different within a row; in each aligned block of 128 rows (0 to 127, 128 to 255, ...) at most 32 rows name the same one
- route_weight: float32 [8192, 4], P(('gr', 'fs')), may hold values from 0.05 to 1
Outputs:
- mixed: bfloat16 [8192, 2048], P(('gr', 'fs'), 'tp')
- gate_packed: bfloat16 [32, 2048, 1024], P('fs', None, 'tp')
- up_packed: bfloat16 [32, 2048, 1024], P('fs', None, 'tp')
- down_packed: bfloat16 [32, 1024, 2048], P('fs', 'tp')
The draws below stay inside these ranges and needn't reach their ends.
Inputs may be any that keep to these rules, and one draw needn't show every extreme that they name: `routes`: each row names 4 different experts. Among the rows of one device no expert is named more than 32 times, and in every draw some expert is named exactly 32 times by the rows of some device.
All inputs are finite; a program needn't handle non-finite values.
Results may differ from the reference program's by a relative error of at most 0.015.
Values may be sent and summed in bfloat16 or wider, within the bound.
No kernel may reach another device: no remote copies, remote signals or barrier semaphores. Data moves between devices by JAX's collectives and lax.ppermute only.
A program may use at most 64 MiB of HBM per device.

```python
import math
import jax
import jax.numpy as jnp
import numpy as np
from jax import lax

D = 2048
FF = 1024
EXPERTS = 32
TOP = 4
TOK_DEV = 128
CAP = 32
TOKENS = 8192
N_TP = 8


def levels(rng, dims, shards, least, top_value):
    def one(position, blocks):
        draws = jax.random.uniform(jax.random.fold_in(jax.random.fold_in(rng, 6), position), (blocks,), jnp.float32, least / len(shards), top_value / len(shards))
        return jnp.repeat(jnp.exp(draws), dims[position] // blocks).reshape((-1,) + (1,) * (len(dims) - position - 1))

    level = one(*shards[0])
    for cut in shards[1:]:
        level = level * one(*cut)
    return level


def assign_block(stream_key, own, number, rows, number_of, top, most, slope):
    sequence = jax.random.permutation(stream_key, number_of)
    heavy_load, usual = load_shares(number_of, rows * top, most, slope, True), load_shares(number_of, rows * top, most, slope, False)
    places = jnp.arange(number_of)

    def named(sizes, rotation):
        used = int((sizes > 0).sum())
        fixed = max(1, used // 4)
        moved = fixed + (places - fixed + rotation * (used - fixed)) % max(1, number_of - fixed)
        return jnp.zeros((number_of,), jnp.int32).at[sequence[jnp.where(places < fixed, places, moved)]].set(jnp.asarray(sizes, jnp.int32))

    sizes = jnp.where(number % 4 == 0, named(heavy_load, number // 4), named(usual, number - number // 4 - 1))
    mixed = jax.random.permutation(jax.random.fold_in(own, 3), number_of)
    source_of, receiver = mixed[0:number_of // 2 * 2:2], mixed[1:number_of // 2 * 2:2]
    room = jnp.minimum(sizes[source_of] - 1, most - sizes[receiver]) // 2
    room = jnp.where((source_of == sequence[0]) | (receiver == sequence[0]) | (sizes[receiver] == 0), 0, jnp.maximum(room, 0))
    moved = jax.random.randint(jax.random.fold_in(own, 4), (number_of // 2,), 0, 1 << 20) % (room + 1)
    sizes = sizes.at[source_of].add(-moved).at[receiver].add(moved)
    members = jnp.searchsorted(jnp.cumsum(sizes), jnp.arange(rows * top), side="right").astype(jnp.int32)
    listing = members.reshape(top, rows).T
    listing = listing[jax.random.permutation(jax.random.fold_in(own, 1), rows)]
    rotation = jax.random.randint(jax.random.fold_in(own, 2), (rows, 1), 0, top)
    return jnp.take_along_axis(listing, (jnp.arange(top)[None, :] + rotation) % top, axis=1)


def load_shares(amount, total, bound, slope, full):
    portions = [(1 << 20) // math.isqrt(standing ** slope) + 1 for standing in range(1, amount + 1)]
    largest = bound if full else min(bound, max(-(-total // amount), total * portions[0] // sum(portions)))
    least = 1 if total - largest >= amount - 1 else 0
    holding, rest = [largest] + [least] * (amount - 1), total - largest - least * (amount - 1)
    while rest > 0:
        movable = [i for i in range(1, amount) if holding[i] < largest] or [i for i in range(1, amount) if holding[i] < bound]
        mass, left = sum([portions[i] for i in movable]), rest
        for i in movable:
            extra = min(bound - holding[i], max(1, left * portions[i] // mass), rest)
            holding[i] = holding[i] + extra
            rest = rest - extra
    return np.array(holding)


def gaussian(rng, shape, width, bound, pieces=(), held_as=jnp.bfloat16):
    entries = width * jax.random.normal(rng, shape, jnp.float32)
    if pieces:
        entries = entries * levels(rng, shape, pieces, -0.22, 0.18)
    return jnp.clip(entries, -bound, bound).astype(held_as)


def setup_inputs(seed: int = 0) -> dict:
    splits = jax.random.split(jax.random.key(seed), 8)
    tokens = gaussian(splits[0], (TOKENS, D), 1.0, 6.0, ((0, 64),))
    norm_gain = jnp.clip(1.0 + 0.18 * jax.random.normal(splits[1], (D,), jnp.float32), 0.1, 1.9)
    gate_train = gaussian(splits[2], (EXPERTS, D, FF), (D // 6) ** -0.5, 0.3125, ((1, 64), (2, 8)), jnp.float32)
    up_train = gaussian(splits[3], (EXPERTS, D, FF), (D // 6) ** -0.5, 0.3125, ((1, 64), (2, 8)), jnp.float32)
    down_train = gaussian(splits[4], (EXPERTS, FF, D), (FF * 4) ** -0.5, 0.09375, ((1, 64), (2, 8)), jnp.float32)
    routes_keys = jax.random.split(jax.random.fold_in(splits[5], 1), TOKENS // TOK_DEV)
    routes_turns = jax.random.permutation(jax.random.fold_in(splits[5], 3), TOKENS // TOK_DEV)
    routes = jax.vmap(lambda own, number: assign_block(jax.random.fold_in(splits[5], 2), own, number, TOK_DEV, EXPERTS, TOP, CAP, 2))(routes_keys, routes_turns).reshape((TOKENS, TOP))
    route_weight = jnp.clip(jnp.exp(math.log(1.0) - 2.9957323 * jax.random.uniform(splits[6], (TOKENS, TOP), jnp.float32) ** levels(splits[6], (TOKENS, TOP), ((0, 64),), -0.2, 0.2)), 0.05, 1.0)
    return dict(tokens=tokens, norm_gain=norm_gain, gate_train=gate_train, up_train=up_train, down_train=down_train, routes=routes, route_weight=route_weight)


CLAMP_LIMIT = 7.0
SLOPE_ALPHA = 1.702
NORM_EPSILON = 1e-06

def reference(tokens, norm_gain, gate_train, up_train, down_train, routes, route_weight):
    gate_packed = (norm_gain[None, :, None] * gate_train).astype(jnp.bfloat16)
    up_packed = (norm_gain[None, :, None] * up_train).astype(jnp.bfloat16)
    down_packed = down_train.astype(jnp.bfloat16)
    tokens_wide = tokens.astype(jnp.float32)
    normed = (tokens_wide * lax.rsqrt(lax.optimization_barrier(jnp.mean(tokens_wide * tokens_wide, axis=1, keepdims=True)) + NORM_EPSILON)).astype(jnp.bfloat16)
    blocks = TOKENS // TOK_DEV
    flat_routes = routes.reshape(blocks, TOK_DEV * TOP)
    one_hot = (flat_routes[:, :, None] == jnp.arange(EXPERTS, dtype=jnp.int32)[None, None, :]).astype(jnp.int32)
    counts = jnp.cumsum(one_hot, axis=1)
    slot_index = lax.optimization_barrier(jnp.sum((counts - 1) * one_hot, axis=2))
    expert_rows = blocks * CAP
    target_rows = (flat_routes * expert_rows + jnp.arange(blocks, dtype=jnp.int32)[:, None] * CAP + slot_index).reshape(-1).astype(jnp.int32)
    copied_rows = jnp.repeat(normed, TOP, axis=0)
    dispatch_buffer = jnp.zeros((EXPERTS * expert_rows, D), jnp.bfloat16).at[target_rows].set(copied_rows)
    dispatch_buffer = dispatch_buffer.reshape(EXPERTS, expert_rows, D)
    block_width = FF // N_TP

    def expert(operands):
        inputs, gate_weight, up_weight, down_weight = operands
        gate_pre = jnp.dot(inputs, gate_weight, preferred_element_type=jnp.float32)
        up_pre = jnp.dot(inputs, up_weight, preferred_element_type=jnp.float32)
        clipped = jnp.minimum(gate_pre, CLAMP_LIMIT)
        hidden = ((jnp.clip(up_pre, -CLAMP_LIMIT, CLAMP_LIMIT) + 1.0) * clipped * jax.nn.sigmoid(SLOPE_ALPHA * clipped)).astype(jnp.bfloat16)
        summed = jnp.zeros((inputs.shape[0], D), jnp.float32)
        for block in range(N_TP):
            partial_value = jnp.dot(hidden[:, block * block_width:(block + 1) * block_width], down_weight[block * block_width:(block + 1) * block_width], preferred_element_type=jnp.float32).astype(jnp.bfloat16)
            partial_value = lax.optimization_barrier(partial_value)
            summed = summed + partial_value.astype(jnp.float32)
        return summed.astype(jnp.bfloat16)
    results = lax.map(expert, (dispatch_buffer, gate_packed, up_packed, down_packed))
    picked = results.reshape(EXPERTS * expert_rows, D)[target_rows].reshape(TOKENS, TOP, D).astype(jnp.float32)
    mixed = lax.optimization_barrier(jnp.sum(picked * route_weight[:, :, None], axis=1)).astype(jnp.bfloat16)
    return (mixed, gate_packed, up_packed, down_packed)
```

```python
import jax
import jax.numpy as jnp
from jax import lax
from jax.sharding import Mesh
from jax.sharding import PartitionSpec as P

CAP = 32
CLAMP_LIMIT = 7.0
SLOPE_ALPHA = 1.702
NORM_EPSILON = 1e-06

GR, ZL, Y, X, C = 2, 8, 4, 4, 2

BF = jnp.bfloat16
F32 = jnp.float32


def ring(k):
    return [(i, (i + k) % Y) for i in range(Y)]


def to_experts_column(pieces, sign=1):
    return [pieces[0]] + [lax.ppermute(pieces[j], "y", ring(sign * j)) for j in range(1, Y)]


def body(tokens, norm_gain, gate_train, up_train, down_train, routes, route_weight):
    iy = lax.axis_index("y")
    n_tok, width = tokens.shape
    part = width // (X * C)

    order = jnp.arange(ZL * Y, dtype=jnp.int32)
    expert = (order % ZL) * Y + (iy + order // ZL) % Y
    hit = routes.T[None, :, :] == expert[:, None, None]
    member = jnp.any(hit, axis=1)
    weight = jnp.sum(jnp.where(hit, route_weight.T[None, :, :], 0.0), axis=1)
    earlier = (jnp.arange(n_tok)[:, None] < jnp.arange(n_tok)[None, :]).astype(BF)
    rank = jnp.dot(member.astype(BF), earlier, preferred_element_type=F32).astype(jnp.int32)
    place = jnp.where(member, rank, -1)
    at_slot = place[:, None, :] == jnp.arange(CAP, dtype=jnp.int32)[None, :, None]
    pick = at_slot.astype(BF).reshape(ZL * Y * CAP, n_tok)
    spread = jnp.where(at_slot, weight[:, None, :], 0.0).reshape(ZL * Y * CAP, n_tok)

    wide = tokens.astype(F32)
    scale = lax.rsqrt(jnp.mean(wide * wide, axis=1, keepdims=True) + NORM_EPSILON)
    start = (lax.axis_index("x") * C + lax.axis_index("c")) * part
    own = lax.dynamic_slice_in_dim(tokens, start, part, 1).astype(F32)
    normed = (own * scale).astype(BF)
    slots = jnp.dot(pick, normed, preferred_element_type=F32).astype(BF)
    slots = slots.reshape(Y, ZL, CAP, part)

    sent = to_experts_column([slots[j] for j in range(Y)])
    rows = jnp.concatenate(sent, axis=1)
    arrived = lax.all_to_all(rows, "zl", split_axis=0, concat_axis=0, tiled=True)
    arrived = arrived.reshape(ZL * Y * CAP, part)
    arrived_all = lax.all_gather(arrived, ("x", "c"), axis=1, tiled=True)

    gain = norm_gain[None, :, None]

    def column(j):
        at = (iy + j) % Y

        def take(a):
            cut = a.reshape(ZL, Y, a.shape[1], a.shape[2])
            return lax.dynamic_index_in_dim(cut, at, 1, keepdims=False)

        both = jnp.concatenate(
            [(gain * take(gate_train)).astype(BF), (gain * take(up_train)).astype(BF)], axis=2
        )
        return jnp.concatenate([both, take(down_train).astype(BF)], axis=1)

    got = to_experts_column([column(j) for j in range(Y)])
    by_offset = jnp.stack([got[(-j) % Y] for j in range(Y)], axis=1)
    by_source = lax.dynamic_slice_in_dim(
        jnp.concatenate([by_offset, by_offset], axis=1), (Y - iy) % Y, Y, 1
    )
    n_up = gate_train.shape[1]
    n_down = down_train.shape[1]
    up_part = by_source[:, :, :n_up].reshape(ZL, Y * n_up, 2 * gate_train.shape[2])
    down_part = by_source[:, :, n_up:].reshape(ZL, Y * n_down, down_train.shape[2])
    up_part, arrived_dep = lax.optimization_barrier((up_part, arrived))
    served = lax.all_to_all(
        jnp.concatenate([up_part] * GR, axis=0), ("gr", "zl"), split_axis=0, concat_axis=0, tiled=True
    ).reshape(width, 2 * gate_train.shape[2])
    down_part, served = lax.optimization_barrier((down_part, served))
    down_cols = lax.all_to_all(
        jnp.concatenate([down_part] * GR, axis=0), ("gr", "zl"), split_axis=0, concat_axis=0, tiled=True
    ).reshape(GR * ZL * Y * n_down, down_train.shape[2])

    ff = gate_train.shape[2]
    gate_weight = served[None, :, :ff]
    up_weight = served[None, :, ff:]

    pre = jnp.dot(arrived_all, served, preferred_element_type=F32)
    clipped = jnp.minimum(pre[:, :ff], CLAMP_LIMIT)
    hidden = (
        (jnp.clip(pre[:, ff:], -CLAMP_LIMIT, CLAMP_LIMIT) + 1.0)
        * clipped
        * jax.nn.sigmoid(SLOPE_ALPHA * clipped)
    ).astype(BF)
    hidden_all = lax.all_gather(hidden, ("x", "c"), axis=1, tiled=True)

    total = jnp.dot(hidden_all, down_cols, preferred_element_type=F32).astype(BF)

    down_own = lax.all_to_all(
        down_cols.reshape(X * C, ff, down_cols.shape[1]), ("x", "c"), split_axis=0, concat_axis=0, tiled=True
    )
    down_weight = down_own.transpose(1, 0, 2).reshape(1, ff, width)

    back = lax.all_to_all(total.reshape(ZL, Y * CAP, part), "zl", split_axis=0, concat_axis=0, tiled=True)
    back = back.reshape(ZL, Y, CAP, part)
    result = to_experts_column([back[:, j] for j in range(Y)], -1)
    result = jnp.stack(result, axis=0).reshape(Y * ZL * CAP, part)
    high = lax.reduce_precision(spread, 8, 7)
    contract = (((0,), (0,)), ((), ()))
    mixed = lax.dot_general(
        high.astype(BF), result, contract, preferred_element_type=F32
    ) + lax.dot_general((spread - high).astype(BF), result, contract, preferred_element_type=F32)
    return (mixed.astype(BF), gate_weight, up_weight, down_weight)


def solution(mesh):
    fine = Mesh(mesh.devices.reshape(GR, ZL, Y, X, C), ("gr", "zl", "y", "x", "c"))
    rows, tp = ("gr", "zl", "y"), ("x", "c")
    served = ("zl", "y")
    placed = (
        P(rows, None),
        P(rows),
        P(None, rows, tp),
        P(None, rows, tp),
        P(None, rows, tp),
        P(rows, None),
        P(rows, None),
    )
    return jax.shard_map(
        body,
        mesh=fine,
        in_specs=placed,
        out_specs=(
            P(rows, tp),
            P(served, None, tp),
            P(served, None, tp),
            P(served, tp, None),
        ),
        check_vma=False,
    )
```

```python
import jax
import jax.numpy as jnp
from jax import lax
from jax.sharding import Mesh
from jax.sharding import PartitionSpec as P

CAP = 32
CLAMP_LIMIT = 7.0
SLOPE_ALPHA = 1.702
NORM_EPSILON = 1e-06

GR, ZL, Y, X, C = 2, 8, 4, 4, 2
FS = ("zl", "y")

BF = jnp.bfloat16
F32 = jnp.float32


def ring(n, k):
    return [(i, (i + k) % n) for i in range(n)]


def exchange(a, axis):
    return lax.all_to_all(a, axis, split_axis=0, concat_axis=0, tiled=True)


def gather_tp(own):
    mine = [own] + [lax.ppermute(own, "x", ring(X, k)) for k in (1, 3, 2)]
    mine = [mine[0], mine[1], mine[3], mine[2]]
    other = [lax.ppermute(a, "c", ring(C, 1)) for a in mine]
    return [(mine[k], other[k]) for k in range(X)]


def relative(blocks, ix, ic):
    found = []
    for k in range(X):
        row = lax.dynamic_index_in_dim(blocks, (ix + X - k) % X, 0, keepdims=False)
        for s in range(C):
            found.append(lax.dynamic_index_in_dim(row, (ic + s) % C, 0, keepdims=False))
    return jnp.concatenate(found, axis=0)


def layer(tokens, norm_gain, gate_train, up_train, down_train, routes, route_weight):
    ix, iy, ic = lax.axis_index("x"), lax.axis_index("y"), lax.axis_index("c")
    n_tok, width = tokens.shape
    part = width // (X * C)
    n_exp = ZL * Y
    n_up, ff = gate_train.shape[1], gate_train.shape[2]

    hit = routes.T[None, :, :] == jnp.arange(n_exp, dtype=jnp.int32)[:, None, None]
    member = jnp.any(hit, axis=1)
    weight = jnp.sum(jnp.where(hit, route_weight.T[None, :, :], 0.0), axis=1)
    earlier = (jnp.arange(n_tok)[:, None] < jnp.arange(n_tok)[None, :]).astype(BF)
    rank = jnp.dot(member.astype(BF), earlier, preferred_element_type=F32).astype(jnp.int32)
    place = jnp.where(member, rank, -1)
    at_slot = place[:, None, :] == jnp.arange(CAP, dtype=jnp.int32)[None, :, None]
    pick = at_slot.astype(BF).reshape(n_exp * CAP, n_tok)

    wide = tokens.astype(F32)
    scale = lax.rsqrt(jnp.mean(wide * wide, axis=1, keepdims=True) + NORM_EPSILON)
    own = lax.dynamic_slice_in_dim(tokens, (ix * C + ic) * part, part, 1).astype(F32)
    normed = (own * scale).astype(BF)
    slots = jnp.dot(pick, normed, preferred_element_type=F32).astype(BF)
    arrived = exchange(slots.reshape(n_exp, CAP, part), FS)
    arrived = arrived.reshape(n_exp * CAP, part)

    gain = norm_gain[None, :, None]

    def column(j):
        at = (iy + j) % Y

        def take(a):
            cut = a.reshape(ZL, Y, a.shape[1], a.shape[2])
            return lax.dynamic_index_in_dim(cut, at, 1, keepdims=False)

        return jnp.concatenate(
            [(gain * take(gate_train)).astype(BF), (gain * take(up_train)).astype(BF)], axis=2
        )

    got = [column(0)] + [lax.ppermute(column(j), "y", ring(Y, j)) for j in range(1, Y)]
    by_offset = jnp.stack([got[(-j) % Y] for j in range(Y)], axis=1)
    by_source = lax.dynamic_slice_in_dim(
        jnp.concatenate([by_offset, by_offset], axis=1), (Y - iy) % Y, Y, 1
    ).reshape(ZL, Y * n_up, 2 * ff)
    by_source, arrived = lax.optimization_barrier((by_source, arrived))
    served = exchange(jnp.concatenate([by_source] * GR, axis=0), ("gr", "zl"))
    pieces = gather_tp(arrived)
    rows = jnp.concatenate([a for pair in pieces for a in pair], axis=1)

    down_local = down_train.astype(BF)
    down_local, served = lax.optimization_barrier((down_local, served))
    down_cols = exchange(jnp.concatenate([down_local] * GR, axis=0), ("gr",) + FS)
    served = served.reshape(width, 2 * ff)
    gate_weight = served[None, :, :ff]
    up_weight = served[None, :, ff:]

    pre = jnp.dot(
        rows, relative(served.reshape(X, C, part, 2 * ff), ix, ic), preferred_element_type=F32
    )
    clipped = jnp.minimum(pre[:, :ff], CLAMP_LIMIT)
    hidden = (
        (jnp.clip(pre[:, ff:], -CLAMP_LIMIT, CLAMP_LIMIT) + 1.0)
        * clipped
        * jax.nn.sigmoid(SLOPE_ALPHA * clipped)
    ).astype(BF)
    pieces = gather_tp(hidden)
    hidden_all = jnp.concatenate([a for pair in pieces for a in pair], axis=1)

    down_blocks = down_cols.reshape(X, C, ff, part)
    total = jnp.dot(hidden_all, relative(down_blocks, ix, ic), preferred_element_type=F32).astype(BF)
    result = exchange(total.reshape(n_exp, CAP, part), FS)

    kept = lax.dynamic_index_in_dim(down_blocks, ic, 1, keepdims=False)
    given = lax.dynamic_index_in_dim(down_blocks, 1 - ic, 1, keepdims=False)
    taken = lax.ppermute(given, "c", ring(C, 1))
    first = jnp.where(ic == 0, kept, taken)
    second = jnp.where(ic == 0, taken, kept)
    wide_rows = jnp.concatenate([first, second], axis=2)
    cols = []
    for k in range(X):
        block = lax.dynamic_index_in_dim(wide_rows, (ix + k) % X, 0, keepdims=False)
        cols.append(block if k == 0 else lax.ppermute(block, "x", ring(X, k)))
    around = jnp.stack([cols[(-j) % X] for j in range(X)] * 2, axis=0)
    ordered = lax.dynamic_slice_in_dim(around, (X - ix) % X, X, 0)
    down_weight = ordered.transpose(1, 0, 2).reshape(1, ff, width)

    spread = jnp.where(at_slot, weight[:, None, :], 0.0).reshape(n_exp * CAP, n_tok)
    high = lax.reduce_precision(spread, 8, 7)
    contract = (((0,), (0,)), ((), ()))
    result = result.reshape(n_exp * CAP, part)
    mixed = lax.dot_general(
        high.astype(BF), result, contract, preferred_element_type=F32
    ) + lax.dot_general((spread - high).astype(BF), result, contract, preferred_element_type=F32)
    return (mixed.astype(BF), gate_weight, up_weight, down_weight)


def solution(mesh):
    fine = Mesh(mesh.devices.reshape(GR, ZL, Y, X, C), ("gr", "zl", "y", "x", "c"))
    rows, tp = ("gr", "zl", "y"), ("x", "c")
    placed = (
        P(rows, None),
        P(rows),
        P(None, rows, tp),
        P(None, rows, tp),
        P(None, rows, tp),
        P(rows, None),
        P(rows, None),
    )
    return jax.shard_map(
        layer,
        mesh=fine,
        in_specs=placed,
        out_specs=(
            P(rows, tp),
            P(FS, None, tp),
            P(FS, None, tp),
            P(FS, tp, None),
        ),
        check_vma=False,
    )
```

```python
import jax
import jax.numpy as jnp
from jax import lax
from jax.sharding import Mesh
from jax.sharding import PartitionSpec as P


CAP = 32
CLAMP_LIMIT = 7.0
SLOPE_ALPHA = 1.702
NORM_EPSILON = 1e-06

GR, ZL, Y, X, C = 2, 8, 4, 4, 2
FS = ("zl", "y")

BF = jnp.bfloat16
F32 = jnp.float32


def ring(n, k):
    return [(i, (i + k) % n) for i in range(n)]


def exchange(a, axis):
    return lax.all_to_all(a, axis, split_axis=0, concat_axis=0, tiled=True)


def along_x(own):
    sent = {k: lax.ppermute(own, "x", ring(X, k)) for k in (1, 3, 2)}
    return [own, sent[1], sent[2], sent[3]]


def other_core(a):
    return lax.ppermute(a, "c", ring(C, 1))


def relative(blocks, ix, ic):
    found = []
    for k in range(X):
        row = lax.dynamic_index_in_dim(blocks, (ix + X - k) % X, 0, keepdims=False)
        for s in range(C):
            found.append(lax.dynamic_index_in_dim(row, (ic + s) % C, 0, keepdims=False))
    return jnp.concatenate(found, axis=0)


def layer(tokens, norm_gain, gate_train, up_train, down_train, routes, route_weight):
    ix, iy, ic = lax.axis_index("x"), lax.axis_index("y"), lax.axis_index("c")
    n_tok, width = tokens.shape
    part = width // (X * C)
    n_exp = ZL * Y
    n_up, ff, n_down = gate_train.shape[1], gate_train.shape[2], down_train.shape[1]

    hit = routes.T[None, :, :] == jnp.arange(n_exp, dtype=jnp.int32)[:, None, None]
    member = jnp.any(hit, axis=1)
    weight = jnp.sum(jnp.where(hit, route_weight.T[None, :, :], 0.0), axis=1)
    earlier = (jnp.arange(n_tok)[:, None] < jnp.arange(n_tok)[None, :]).astype(BF)
    rank = jnp.dot(member.astype(BF), earlier, preferred_element_type=F32).astype(jnp.int32)
    place = jnp.where(member, rank, -1)
    at_slot = place[:, None, :] == jnp.arange(CAP, dtype=jnp.int32)[None, :, None]
    pick = at_slot.astype(BF).reshape(n_exp * CAP, n_tok)

    wide = tokens.astype(F32)
    scale = lax.rsqrt(jnp.mean(wide * wide, axis=1, keepdims=True) + NORM_EPSILON)
    own = lax.dynamic_slice_in_dim(tokens, (ix * C + ic) * part, part, 1).astype(F32)
    normed = (own * scale).astype(BF)
    slots = jnp.dot(pick, normed, preferred_element_type=F32).astype(BF)
    slots = slots.reshape(n_exp, CAP, part)
    mixed_in = exchange(jnp.concatenate([slots, down_train.astype(BF)], axis=1), FS)
    arrived = mixed_in[:, :CAP].reshape(n_exp * CAP, part)
    down_half = mixed_in[:, CAP:].reshape(n_exp * n_down, part)

    gain = norm_gain[None, :, None]

    def column(j):
        at = (iy + j) % Y

        def take(a):
            cut = a.reshape(ZL, Y, a.shape[1], a.shape[2])
            return lax.dynamic_index_in_dim(cut, at, 1, keepdims=False)

        return jnp.concatenate(
            [(gain * take(gate_train)).astype(BF), (gain * take(up_train)).astype(BF)], axis=2
        )

    got = [column(0)] + [lax.ppermute(column(j), "y", ring(Y, j)) for j in range(1, Y)]
    by_offset = jnp.stack([got[(-j) % Y] for j in range(Y)], axis=1)
    by_source = lax.dynamic_slice_in_dim(
        jnp.concatenate([by_offset, by_offset], axis=1), (Y - iy) % Y, Y, 1
    ).reshape(ZL, Y * n_up, 2 * ff)
    twice = jnp.concatenate([by_source] * GR, axis=0)
    twice, arrived = lax.optimization_barrier((twice, arrived))
    served = exchange(twice, ("gr", "zl"))
    near = along_x(arrived)
    far = {k: other_core(near[k]) for k in (0, 1, 3)}
    down_half, near[2] = lax.optimization_barrier((down_half, near[2]))
    down_other = lax.ppermute(down_half, "gr", ring(GR, 1))
    far[2] = other_core(near[2])
    rows = jnp.concatenate([a for k in range(X) for a in (near[k], far[k])], axis=1)

    served = served.reshape(width, 2 * ff)
    gate_weight = served[None, :, :ff]
    up_weight = served[None, :, ff:]

    pre = jnp.dot(
        rows, relative(served.reshape(X, C, part, 2 * ff), ix, ic), preferred_element_type=F32
    )
    clipped = jnp.minimum(pre[:, :ff], CLAMP_LIMIT)
    hidden = (
        (jnp.clip(pre[:, ff:], -CLAMP_LIMIT, CLAMP_LIMIT) + 1.0)
        * clipped
        * jax.nn.sigmoid(SLOPE_ALPHA * clipped)
    ).astype(BF)
    own_core = exchange(jnp.broadcast_to(hidden[None], (X,) + hidden.shape), "x")
    their_core = other_core(own_core)

    ig = lax.axis_index("gr")
    down_blocks = jnp.concatenate(
        [jnp.where(ig == 0, down_half, down_other), jnp.where(ig == 0, down_other, down_half)], axis=0
    ).reshape(X, C, ff, part)

    def down_of(core):
        return lax.dynamic_index_in_dim(down_blocks, core, 1, keepdims=False).reshape(X * ff, part)

    def flat(a):
        return jnp.concatenate([a[x] for x in range(X)], axis=1)

    total = (
        jnp.dot(flat(own_core), down_of(ic), preferred_element_type=F32)
        + jnp.dot(flat(their_core), down_of(1 - ic), preferred_element_type=F32)
    ).astype(BF)
    total, down_blocks = lax.optimization_barrier((total, down_blocks))
    result = exchange(total.reshape(n_exp, CAP, part), FS)

    kept = lax.dynamic_index_in_dim(down_blocks, ic, 1, keepdims=False)
    given = lax.dynamic_index_in_dim(down_blocks, 1 - ic, 1, keepdims=False)
    taken = lax.ppermute(given, "c", ring(C, 1))
    first = jnp.where(ic == 0, kept, taken)
    second = jnp.where(ic == 0, taken, kept)
    wide_rows = jnp.concatenate([first, second], axis=2)
    cols = []
    for k in range(X):
        block = lax.dynamic_index_in_dim(wide_rows, (ix + k) % X, 0, keepdims=False)
        cols.append(block if k == 0 else lax.ppermute(block, "x", ring(X, k)))
    around = jnp.stack([cols[(-j) % X] for j in range(X)] * 2, axis=0)
    ordered = lax.dynamic_slice_in_dim(around, (X - ix) % X, X, 0)
    down_weight = ordered.transpose(1, 0, 2).reshape(1, ff, width)

    spread = jnp.where(at_slot, weight[:, None, :], 0.0).reshape(n_exp * CAP, n_tok)
    high = lax.reduce_precision(spread, 8, 7)
    contract = (((0,), (0,)), ((), ()))
    result = result.reshape(n_exp * CAP, part)
    mixed = lax.dot_general(
        high.astype(BF), result, contract, preferred_element_type=F32
    ) + lax.dot_general((spread - high).astype(BF), result, contract, preferred_element_type=F32)
    return (mixed.astype(BF), gate_weight, up_weight, down_weight)


def solution(mesh):
    fine = Mesh(mesh.devices.reshape(GR, ZL, Y, X, C), ("gr", "zl", "y", "x", "c"))
    rows, tp = ("gr", "zl", "y"), ("x", "c")
    placed = (
        P(rows, None),
        P(rows),
        P(None, rows, tp),
        P(None, rows, tp),
        P(None, rows, tp),
        P(rows, None),
        P(rows, None),
    )
    return jax.shard_map(
        layer,
        mesh=fine,
        in_specs=placed,
        out_specs=(
            P(rows, tp),
            P(FS, None, tp),
            P(FS, None, tp),
            P(FS, tp, None),
        ),
        check_vma=False,
    )
```

```python
import jax
import jax.numpy as jnp
from jax import lax
from jax.sharding import Mesh
from jax.sharding import PartitionSpec as P


CAP = 32
CLAMP_LIMIT = 7.0
SLOPE_ALPHA = 1.702
NORM_EPSILON = 1e-06

GR, ZL, Y, X, C = 2, 8, 4, 4, 2
FS = ("zl", "y")

BF = jnp.bfloat16
F32 = jnp.float32


def ring(n, k):
    return [(i, (i + k) % n) for i in range(n)]


def exchange(a, axis):
    return lax.all_to_all(a, axis, split_axis=0, concat_axis=0, tiled=True)


def gather_tp(own):
    mine = [own] + [lax.ppermute(own, "x", ring(X, k)) for k in (1, 3, 2)]
    mine = [mine[0], mine[1], mine[3], mine[2]]
    other = [lax.ppermute(a, "c", ring(C, 1)) for a in mine]
    return [(mine[k], other[k]) for k in range(X)]


def relative(blocks, ix, ic):
    found = []
    for k in range(X):
        row = lax.dynamic_index_in_dim(blocks, (ix + X - k) % X, 0, keepdims=False)
        for s in range(C):
            found.append(lax.dynamic_index_in_dim(row, (ic + s) % C, 0, keepdims=False))
    return jnp.concatenate(found, axis=0)


def layer(tokens, norm_gain, gate_train, up_train, down_train, routes, route_weight):
    ix, iy, ic = lax.axis_index("x"), lax.axis_index("y"), lax.axis_index("c")
    n_tok, width = tokens.shape
    part = width // (X * C)
    n_exp = ZL * Y
    n_up, ff, n_down = gate_train.shape[1], gate_train.shape[2], down_train.shape[1]

    hit = routes.T[None, :, :] == jnp.arange(n_exp, dtype=jnp.int32)[:, None, None]
    member = jnp.any(hit, axis=1)
    weight = jnp.sum(jnp.where(hit, route_weight.T[None, :, :], 0.0), axis=1)
    earlier = (jnp.arange(n_tok)[:, None] < jnp.arange(n_tok)[None, :]).astype(BF)
    rank = jnp.dot(member.astype(BF), earlier, preferred_element_type=F32).astype(jnp.int32)
    place = jnp.where(member, rank, -1)
    at_slot = place[:, None, :] == jnp.arange(CAP, dtype=jnp.int32)[None, :, None]
    pick = at_slot.astype(BF).reshape(n_exp * CAP, n_tok)

    wide = tokens.astype(F32)
    scale = lax.rsqrt(jnp.mean(wide * wide, axis=1, keepdims=True) + NORM_EPSILON)
    own = lax.dynamic_slice_in_dim(tokens, (ix * C + ic) * part, part, 1).astype(F32)
    normed = (own * scale).astype(BF)
    slots = jnp.dot(pick, normed, preferred_element_type=F32).astype(BF)
    arrived = exchange(slots.reshape(n_exp, CAP, part), FS)
    arrived = arrived.reshape(n_exp * CAP, part)

    gain = norm_gain[None, :, None]

    def column(j):
        at = (iy + j) % Y

        def take(a):
            cut = a.reshape(ZL, Y, a.shape[1], a.shape[2])
            return lax.dynamic_index_in_dim(cut, at, 1, keepdims=False)

        both = jnp.concatenate(
            [(gain * take(gate_train)).astype(BF), (gain * take(up_train)).astype(BF)], axis=2
        )
        return jnp.concatenate([both, take(down_train).astype(BF)], axis=1)

    got = [column(0)] + [lax.ppermute(column(j), "y", ring(Y, j)) for j in range(1, Y)]
    by_offset = jnp.stack([got[(-j) % Y] for j in range(Y)], axis=1)
    by_source = lax.dynamic_slice_in_dim(
        jnp.concatenate([by_offset, by_offset], axis=1), (Y - iy) % Y, Y, 1
    )
    down_part = by_source[:, :, n_up:].reshape(ZL, Y * n_down, part)
    down_twice = jnp.concatenate([down_part] * GR, axis=0)
    by_source = by_source[:, :, :n_up].reshape(ZL, Y * n_up, 2 * ff)
    twice, arrived = lax.optimization_barrier((jnp.concatenate([by_source] * GR, axis=0), arrived))
    served = exchange(twice, ("gr", "zl"))
    pieces = gather_tp(arrived)
    rows = jnp.concatenate([a for pair in pieces for a in pair], axis=1)

    served = served.reshape(width, 2 * ff)
    gate_weight = served[None, :, :ff]
    up_weight = served[None, :, ff:]

    pre = jnp.dot(
        rows, relative(served.reshape(X, C, part, 2 * ff), ix, ic), preferred_element_type=F32
    )
    clipped = jnp.minimum(pre[:, :ff], CLAMP_LIMIT)
    hidden = (
        (jnp.clip(pre[:, ff:], -CLAMP_LIMIT, CLAMP_LIMIT) + 1.0)
        * clipped
        * jax.nn.sigmoid(SLOPE_ALPHA * clipped)
    ).astype(BF)
    down_twice, hidden = lax.optimization_barrier((down_twice, hidden))
    down_cols = exchange(down_twice, ("gr", "zl"))
    pieces = gather_tp(hidden)
    hidden_all = jnp.concatenate([a for pair in pieces for a in pair], axis=1)

    down_blocks = down_cols.reshape(X, C, ff, part)
    total = jnp.dot(hidden_all, relative(down_blocks, ix, ic), preferred_element_type=F32).astype(BF)
    total, down_blocks = lax.optimization_barrier((total, down_blocks))
    result = exchange(total.reshape(n_exp, CAP, part), FS)

    kept = lax.dynamic_index_in_dim(down_blocks, ic, 1, keepdims=False)
    given = lax.dynamic_index_in_dim(down_blocks, 1 - ic, 1, keepdims=False)
    taken = lax.ppermute(given, "c", ring(C, 1))
    first = jnp.where(ic == 0, kept, taken)
    second = jnp.where(ic == 0, taken, kept)
    wide_rows = jnp.concatenate([first, second], axis=2)
    cols = []
    for k in range(X):
        block = lax.dynamic_index_in_dim(wide_rows, (ix + k) % X, 0, keepdims=False)
        cols.append(block if k == 0 else lax.ppermute(block, "x", ring(X, k)))
    around = jnp.stack([cols[(-j) % X] for j in range(X)] * 2, axis=0)
    ordered = lax.dynamic_slice_in_dim(around, (X - ix) % X, X, 0)
    down_weight = ordered.transpose(1, 0, 2).reshape(1, ff, width)

    spread = jnp.where(at_slot, weight[:, None, :], 0.0).reshape(n_exp * CAP, n_tok)
    high = lax.reduce_precision(spread, 8, 7)
    contract = (((0,), (0,)), ((), ()))
    result = result.reshape(n_exp * CAP, part)
    mixed = lax.dot_general(
        high.astype(BF), result, contract, preferred_element_type=F32
    ) + lax.dot_general((spread - high).astype(BF), result, contract, preferred_element_type=F32)
    return (mixed.astype(BF), gate_weight, up_weight, down_weight)


def solution(mesh):
    fine = Mesh(mesh.devices.reshape(GR, ZL, Y, X, C), ("gr", "zl", "y", "x", "c"))
    rows, tp = ("gr", "zl", "y"), ("x", "c")
    placed = (
        P(rows, None),
        P(rows),
        P(None, rows, tp),
        P(None, rows, tp),
        P(None, rows, tp),
        P(rows, None),
        P(rows, None),
    )
    return jax.shard_map(
        layer,
        mesh=fine,
        in_specs=placed,
        out_specs=(
            P(rows, tp),
            P(FS, None, tp),
            P(FS, None, tp),
            P(FS, tp, None),
        ),
        check_vma=False,
    )
```

```python
import jax
import jax.numpy as jnp
from jax import lax
from jax.sharding import Mesh
from jax.sharding import PartitionSpec as P


CAP = 32
CLAMP_LIMIT = 7.0
SLOPE_ALPHA = 1.702
NORM_EPSILON = 1e-06

GR, ZL, Y, X, C = 2, 8, 4, 4, 2
FS = ("zl", "y")

BF = jnp.bfloat16
F32 = jnp.float32


def ring(n, k):
    return [(i, (i + k) % n) for i in range(n)]


def exchange(a, axis):
    return lax.all_to_all(a, axis, split_axis=0, concat_axis=0, tiled=True)


def gather_tp(own):
    mine = [own] + [lax.ppermute(own, "x", ring(X, k)) for k in (1, 3, 2)]
    mine = [mine[0], mine[1], mine[3], mine[2]]
    other = [lax.ppermute(a, "c", ring(C, 1)) for a in mine]
    return [(mine[k], other[k]) for k in range(X)]


def relative(blocks, ix, ic):
    found = []
    for k in range(X):
        row = lax.dynamic_index_in_dim(blocks, (ix + X - k) % X, 0, keepdims=False)
        for s in range(C):
            found.append(lax.dynamic_index_in_dim(row, (ic + s) % C, 0, keepdims=False))
    return jnp.concatenate(found, axis=0)


def matched(pieces, blocks, ix, ic):
    total = None
    for k in range(X):
        row = lax.dynamic_index_in_dim(blocks, (ix + X - k) % X, 0, keepdims=False)
        for s in range(C):
            block = lax.dynamic_index_in_dim(row, (ic + s) % C, 0, keepdims=False)
            term = jnp.dot(pieces[k][s], block, preferred_element_type=F32)
            total = term if total is None else total + term
    return total


def layer(tokens, norm_gain, gate_train, up_train, down_train, routes, route_weight):
    ix, iy, ic = lax.axis_index("x"), lax.axis_index("y"), lax.axis_index("c")
    n_tok, width = tokens.shape
    part = width // (X * C)
    n_exp = ZL * Y
    n_up, ff, n_down = gate_train.shape[1], gate_train.shape[2], down_train.shape[1]

    hit = routes.T[None, :, :] == jnp.arange(n_exp, dtype=jnp.int32)[:, None, None]
    member = jnp.any(hit, axis=1)
    weight = jnp.sum(jnp.where(hit, route_weight.T[None, :, :], 0.0), axis=1)
    earlier = (jnp.arange(n_tok)[:, None] < jnp.arange(n_tok)[None, :]).astype(BF)
    rank = jnp.dot(member.astype(BF), earlier, preferred_element_type=F32).astype(jnp.int32)
    place = jnp.where(member, rank, -1)
    at_slot = place[:, None, :] == jnp.arange(CAP, dtype=jnp.int32)[None, :, None]
    pick = at_slot.astype(BF).reshape(n_exp * CAP, n_tok)

    wide = tokens.astype(F32)
    scale = lax.rsqrt(jnp.mean(wide * wide, axis=1, keepdims=True) + NORM_EPSILON)
    own = lax.dynamic_slice_in_dim(tokens, (ix * C + ic) * part, part, 1).astype(F32)
    normed = (own * scale).astype(BF)
    slots = jnp.dot(pick, normed, preferred_element_type=F32).astype(BF)
    arrived = exchange(slots.reshape(n_exp, CAP, part), FS)
    arrived = arrived.reshape(n_exp * CAP, part)

    gain = norm_gain[None, :, None]

    def column(j):
        at = (iy + j) % Y

        def take(a):
            cut = a.reshape(ZL, Y, a.shape[1], a.shape[2])
            return lax.dynamic_index_in_dim(cut, at, 1, keepdims=False)

        both = jnp.concatenate(
            [(gain * take(gate_train)).astype(BF), (gain * take(up_train)).astype(BF)], axis=2
        )
        return jnp.concatenate([both, take(down_train).astype(BF)], axis=1)

    got = [column(0)] + [lax.ppermute(column(j), "y", ring(Y, j)) for j in range(1, Y)]
    by_offset = jnp.stack([got[(-j) % Y] for j in range(Y)], axis=1)
    by_source = lax.dynamic_slice_in_dim(
        jnp.concatenate([by_offset, by_offset], axis=1), (Y - iy) % Y, Y, 1
    )
    down_part = by_source[:, :, n_up:].reshape(ZL, Y * n_down, part)
    down_twice = jnp.concatenate([down_part] * GR, axis=0)
    by_source = by_source[:, :, :n_up].reshape(ZL, Y * n_up, 2 * ff)
    twice, arrived = lax.optimization_barrier((jnp.concatenate([by_source] * GR, axis=0), arrived))
    served = exchange(twice, ("gr", "zl"))
    pieces = gather_tp(arrived)
    rows = jnp.concatenate([a for pair in pieces for a in pair], axis=1)

    down_twice, served = lax.optimization_barrier((down_twice, served))
    down_cols = exchange(down_twice, ("gr", "zl"))
    served = served.reshape(width, 2 * ff)
    gate_weight = served[None, :, :ff]
    up_weight = served[None, :, ff:]

    pre = jnp.dot(
        rows, relative(served.reshape(X, C, part, 2 * ff), ix, ic), preferred_element_type=F32
    )
    clipped = jnp.minimum(pre[:, :ff], CLAMP_LIMIT)
    hidden = (
        (jnp.clip(pre[:, ff:], -CLAMP_LIMIT, CLAMP_LIMIT) + 1.0)
        * clipped
        * jax.nn.sigmoid(SLOPE_ALPHA * clipped)
    ).astype(BF)
    near = [hidden, None, None, None]
    for k in (1, 3, 2):
        near[k] = lax.ppermute(hidden, "x", ring(X, k))
    other = [lax.ppermute(a, "c", ring(C, 1)) for a in near]
    pairs = [(near[k], other[k]) for k in range(X)]

    down_blocks = down_cols.reshape(X, C, ff, part)
    total = matched(pairs, down_blocks, ix, ic).astype(BF)
    total, down_blocks = lax.optimization_barrier((total, down_blocks))
    result = exchange(total.reshape(n_exp, CAP, part), FS)

    kept = lax.dynamic_index_in_dim(down_blocks, ic, 1, keepdims=False)
    given = lax.dynamic_index_in_dim(down_blocks, 1 - ic, 1, keepdims=False)
    taken = lax.ppermute(given, "c", ring(C, 1))
    first = jnp.where(ic == 0, kept, taken)
    second = jnp.where(ic == 0, taken, kept)
    wide_rows = jnp.concatenate([first, second], axis=2)
    cols = []
    for k in range(X):
        block = lax.dynamic_index_in_dim(wide_rows, (ix + k) % X, 0, keepdims=False)
        cols.append(block if k == 0 else lax.ppermute(block, "x", ring(X, k)))
    around = jnp.stack([cols[(-j) % X] for j in range(X)] * 2, axis=0)
    ordered = lax.dynamic_slice_in_dim(around, (X - ix) % X, X, 0)
    down_weight = ordered.transpose(1, 0, 2).reshape(1, ff, width)

    spread = jnp.where(at_slot, weight[:, None, :], 0.0).reshape(n_exp * CAP, n_tok)
    high = lax.reduce_precision(spread, 8, 7)
    contract = (((0,), (0,)), ((), ()))
    result = result.reshape(n_exp * CAP, part)
    mixed = lax.dot_general(
        high.astype(BF), result, contract, preferred_element_type=F32
    ) + lax.dot_general((spread - high).astype(BF), result, contract, preferred_element_type=F32)
    return (mixed.astype(BF), gate_weight, up_weight, down_weight)


def solution(mesh):
    fine = Mesh(mesh.devices.reshape(GR, ZL, Y, X, C), ("gr", "zl", "y", "x", "c"))
    rows, tp = ("gr", "zl", "y"), ("x", "c")
    placed = (
        P(rows, None),
        P(rows),
        P(None, rows, tp),
        P(None, rows, tp),
        P(None, rows, tp),
        P(rows, None),
        P(rows, None),
    )
    return jax.shard_map(
        layer,
        mesh=fine,
        in_specs=placed,
        out_specs=(
            P(rows, tp),
            P(FS, None, tp),
            P(FS, None, tp),
            P(FS, tp, None),
        ),
        check_vma=False,
    )
```

```python
import jax
import jax.numpy as jnp
from jax import lax
from jax.sharding import Mesh
from jax.sharding import PartitionSpec as P


CAP = 32
CLAMP_LIMIT = 7.0
SLOPE_ALPHA = 1.702
NORM_EPSILON = 1e-06

GR, ZL, Y, X, C = 2, 8, 4, 4, 2
FS = ("zl", "y")

BF = jnp.bfloat16
F32 = jnp.float32


def ring(n, k):
    return [(i, (i + k) % n) for i in range(n)]


def exchange(a, axis):
    return lax.all_to_all(a, axis, split_axis=0, concat_axis=0, tiled=True)


def gather_tp(own):
    mine = [own] + [lax.ppermute(own, "x", ring(X, k)) for k in (1, 3, 2)]
    mine = [mine[0], mine[1], mine[3], mine[2]]
    other = [lax.ppermute(a, "c", ring(C, 1)) for a in mine]
    return [(mine[k], other[k]) for k in range(X)]


def relative(blocks, ix, ic):
    found = []
    for k in range(X):
        row = lax.dynamic_index_in_dim(blocks, (ix + X - k) % X, 0, keepdims=False)
        for s in range(C):
            found.append(lax.dynamic_index_in_dim(row, (ic + s) % C, 0, keepdims=False))
    return jnp.concatenate(found, axis=0)


def matched(pieces, blocks, ix, ic):
    total = None
    for k in range(X):
        row = lax.dynamic_index_in_dim(blocks, (ix + X - k) % X, 0, keepdims=False)
        for s in range(C):
            block = lax.dynamic_index_in_dim(row, (ic + s) % C, 0, keepdims=False)
            term = jnp.dot(pieces[k][s], block, preferred_element_type=F32)
            total = term if total is None else total + term
    return total


def layer(tokens, norm_gain, gate_train, up_train, down_train, routes, route_weight):
    ix, iy, ic = lax.axis_index("x"), lax.axis_index("y"), lax.axis_index("c")
    n_tok, width = tokens.shape
    part = width // (X * C)
    n_exp = ZL * Y
    n_up, ff, n_down = gate_train.shape[1], gate_train.shape[2], down_train.shape[1]

    hit = routes.T[None, :, :] == jnp.arange(n_exp, dtype=jnp.int32)[:, None, None]
    member = jnp.any(hit, axis=1)
    weight = jnp.sum(jnp.where(hit, route_weight.T[None, :, :], 0.0), axis=1)
    earlier = (jnp.arange(n_tok)[:, None] < jnp.arange(n_tok)[None, :]).astype(BF)
    rank = jnp.dot(member.astype(BF), earlier, preferred_element_type=F32).astype(jnp.int32)
    place = jnp.where(member, rank, -1)
    at_slot = place[:, None, :] == jnp.arange(CAP, dtype=jnp.int32)[None, :, None]
    pick = at_slot.astype(BF).reshape(n_exp * CAP, n_tok)

    wide = lax.optimization_barrier(tokens.astype(F32))
    scale = lax.rsqrt(jnp.mean(wide * wide, axis=1, keepdims=True) + NORM_EPSILON)
    own = lax.dynamic_slice_in_dim(wide, (ix * C + ic) * part, part, 1)
    normed = (own * scale).astype(BF)
    slots = jnp.dot(pick, normed, preferred_element_type=F32).astype(BF)
    arrived = exchange(slots.reshape(n_exp, CAP, part), FS)
    arrived = arrived.reshape(n_exp * CAP, part)

    gain = norm_gain[None, :, None]

    def column(j):
        at = (iy + j) % Y

        def take(a):
            cut = a.reshape(ZL, Y, a.shape[1], a.shape[2])
            return lax.dynamic_index_in_dim(cut, at, 1, keepdims=False)

        both = jnp.concatenate(
            [(gain * take(gate_train)).astype(BF), (gain * take(up_train)).astype(BF)], axis=2
        )
        return jnp.concatenate([both, take(down_train).astype(BF)], axis=1)

    got = [column(0)] + [lax.ppermute(column(j), "y", ring(Y, j)) for j in range(1, Y)]
    by_offset = jnp.stack([got[(-j) % Y] for j in range(Y)], axis=1)
    by_source = lax.dynamic_slice_in_dim(
        jnp.concatenate([by_offset, by_offset], axis=1), (Y - iy) % Y, Y, 1
    )
    down_part = by_source[:, :, n_up:].reshape(ZL, Y * n_down, part)
    down_twice = jnp.concatenate([down_part] * GR, axis=0)
    by_source = by_source[:, :, :n_up].reshape(ZL, Y * n_up, 2 * ff)
    twice, arrived = lax.optimization_barrier((jnp.concatenate([by_source] * GR, axis=0), arrived))
    served = exchange(twice, ("gr", "zl"))
    pieces = gather_tp(arrived)
    rows = jnp.concatenate([a for pair in pieces for a in pair], axis=1)

    down_twice, served = lax.optimization_barrier((down_twice, served))
    down_cols = exchange(down_twice, ("gr", "zl"))
    served = served.reshape(width, 2 * ff)
    gate_weight = served[None, :, :ff]
    up_weight = served[None, :, ff:]

    pre = jnp.dot(
        rows, relative(served.reshape(X, C, part, 2 * ff), ix, ic), preferred_element_type=F32
    )
    clipped = jnp.minimum(pre[:, :ff], CLAMP_LIMIT)
    hidden = (
        (jnp.clip(pre[:, ff:], -CLAMP_LIMIT, CLAMP_LIMIT) + 1.0)
        * clipped
        * jax.nn.sigmoid(SLOPE_ALPHA * clipped)
    ).astype(BF)
    near = [hidden, None, None, None]
    for k in (1, 3, 2):
        near[k] = lax.ppermute(hidden, "x", ring(X, k))
    other = [lax.ppermute(a, "c", ring(C, 1)) for a in near]
    pairs = [(near[k], other[k]) for k in range(X)]

    down_blocks = down_cols.reshape(X, C, ff, part)
    total = matched(pairs, down_blocks, ix, ic).astype(BF)
    total, down_blocks = lax.optimization_barrier((total, down_blocks))
    result = exchange(total.reshape(n_exp, CAP, part), FS)

    kept = lax.dynamic_index_in_dim(down_blocks, ic, 1, keepdims=False)
    given = lax.dynamic_index_in_dim(down_blocks, 1 - ic, 1, keepdims=False)
    taken = lax.ppermute(given, "c", ring(C, 1))
    first = jnp.where(ic == 0, kept, taken)
    second = jnp.where(ic == 0, taken, kept)
    wide_rows = jnp.concatenate([first, second], axis=2)
    cols = []
    for k in range(X):
        block = lax.dynamic_index_in_dim(wide_rows, (ix + k) % X, 0, keepdims=False)
        cols.append(block if k == 0 else lax.ppermute(block, "x", ring(X, k)))
    around = jnp.stack([cols[(-j) % X] for j in range(X)] * 2, axis=0)
    ordered = lax.dynamic_slice_in_dim(around, (X - ix) % X, X, 0)
    down_weight = ordered.transpose(1, 0, 2).reshape(1, ff, width)

    spread = jnp.where(at_slot, weight[:, None, :], 0.0).reshape(n_exp * CAP, n_tok)
    high = lax.reduce_precision(spread, 8, 7)
    contract = (((0,), (0,)), ((), ()))
    result = result.reshape(n_exp * CAP, part)
    coefficients = jnp.concatenate([high.astype(BF), (spread - high).astype(BF)], axis=1)
    coefficients, total = lax.optimization_barrier((coefficients, total))
    products = lax.dot_general(coefficients, result, contract, preferred_element_type=F32)
    mixed = products[:n_tok] + products[n_tok:]
    return (mixed.astype(BF), gate_weight, up_weight, down_weight)


def solution(mesh):
    fine = Mesh(mesh.devices.reshape(GR, ZL, Y, X, C), ("gr", "zl", "y", "x", "c"))
    rows, tp = ("gr", "zl", "y"), ("x", "c")
    placed = (
        P(rows, None),
        P(rows),
        P(None, rows, tp),
        P(None, rows, tp),
        P(None, rows, tp),
        P(rows, None),
        P(rows, None),
    )
    return jax.shard_map(
        layer,
        mesh=fine,
        in_specs=placed,
        out_specs=(
            P(rows, tp),
            P(FS, None, tp),
            P(FS, None, tp),
            P(FS, tp, None),
        ),
        check_vma=False,
    )
```

```python
import jax
import jax.numpy as jnp
from jax import lax
from jax.sharding import Mesh
from jax.sharding import PartitionSpec as P


CAP = 32
CLAMP_LIMIT = 7.0
SLOPE_ALPHA = 1.702
NORM_EPSILON = 1e-06

GR, ZL, Y, X, C = 2, 8, 4, 4, 2
FS = ("zl", "y")

BF = jnp.bfloat16
F32 = jnp.float32


def ring(n, k):
    return [(i, (i + k) % n) for i in range(n)]


def exchange(a, axis):
    return lax.all_to_all(a, axis, split_axis=0, concat_axis=0, tiled=True)


def gather_tp(own):
    mine = [own] + [lax.ppermute(own, "x", ring(X, k)) for k in (1, 3, 2)]
    mine = [mine[0], mine[1], mine[3], mine[2]]
    other = [lax.ppermute(a, "c", ring(C, 1)) for a in mine]
    return [(mine[k], other[k]) for k in range(X)]


def relative(blocks, ix, ic):
    found = []
    for k in range(X):
        row = lax.dynamic_index_in_dim(blocks, (ix + X - k) % X, 0, keepdims=False)
        for s in range(C):
            found.append(lax.dynamic_index_in_dim(row, (ic + s) % C, 0, keepdims=False))
    return jnp.concatenate(found, axis=0)


def matched(pieces, blocks, ix, ic):
    total = None
    for k in range(X):
        row = lax.dynamic_index_in_dim(blocks, (ix + X - k) % X, 0, keepdims=False)
        for s in range(C):
            block = lax.dynamic_index_in_dim(row, (ic + s) % C, 0, keepdims=False)
            term = jnp.dot(pieces[k][s], block, preferred_element_type=F32)
            total = term if total is None else total + term
    return total


def layer(tokens, norm_gain, gate_train, up_train, down_train, routes, route_weight):
    ix, iy, ic = lax.axis_index("x"), lax.axis_index("y"), lax.axis_index("c")
    n_tok, width = tokens.shape
    part = width // (X * C)
    n_exp = ZL * Y
    n_up, ff, n_down = gate_train.shape[1], gate_train.shape[2], down_train.shape[1]

    hit = routes.T[None, :, :] == jnp.arange(n_exp, dtype=jnp.int32)[:, None, None]
    member = jnp.any(hit, axis=1)
    weight = jnp.sum(jnp.where(hit, route_weight.T[None, :, :], 0.0), axis=1)
    earlier = (jnp.arange(n_tok)[:, None] < jnp.arange(n_tok)[None, :]).astype(BF)
    rank = jnp.dot(member.astype(BF), earlier, preferred_element_type=F32).astype(jnp.int32)
    place = jnp.where(member, rank, -1)
    at_slot = place[:, None, :] == jnp.arange(CAP, dtype=jnp.int32)[None, :, None]
    pick = at_slot.astype(BF).reshape(n_exp * CAP, n_tok)

    wide = lax.optimization_barrier(tokens.astype(F32))
    scale = lax.rsqrt(jnp.mean(wide * wide, axis=1, keepdims=True) + NORM_EPSILON)
    own = lax.dynamic_slice_in_dim(wide, (ix * C + ic) * part, part, 1)
    normed = (own * scale).astype(BF)
    slots = jnp.dot(pick, normed, preferred_element_type=F32).astype(BF)
    arrived = exchange(slots.reshape(n_exp, CAP, part), FS)
    arrived = arrived.reshape(n_exp * CAP, part)

    gain = norm_gain[None, :, None]

    def column(j):
        at = (iy + j) % Y

        def take(a):
            cut = a.reshape(ZL, Y, a.shape[1], a.shape[2])
            return lax.dynamic_index_in_dim(cut, at, 1, keepdims=False)

        both = jnp.concatenate(
            [(gain * take(gate_train)).astype(BF), (gain * take(up_train)).astype(BF)], axis=2
        )
        return jnp.concatenate([both, take(down_train).astype(BF)], axis=1)

    got = [column(0)] + [lax.ppermute(column(j), "y", ring(Y, j)) for j in range(1, Y)]
    by_offset = jnp.stack([got[(-j) % Y] for j in range(Y)], axis=1)
    by_source = lax.dynamic_slice_in_dim(
        jnp.concatenate([by_offset, by_offset], axis=1), (Y - iy) % Y, Y, 1
    )
    down_part = by_source[:, :, n_up:].reshape(ZL, Y * n_down, part)
    down_twice = jnp.concatenate([down_part] * GR, axis=0)
    by_source = by_source[:, :, :n_up].reshape(ZL, Y * n_up, 2 * ff)
    twice, arrived = lax.optimization_barrier((jnp.concatenate([by_source] * GR, axis=0), arrived))
    served = exchange(twice, ("gr", "zl"))
    pieces = gather_tp(arrived)
    rows = jnp.concatenate([a for pair in pieces for a in pair], axis=1)

    down_twice, served = lax.optimization_barrier((down_twice, served))
    down_cols = exchange(down_twice, ("gr", "zl"))
    served = served.reshape(width, 2 * ff)
    gate_weight = served[None, :, :ff]
    up_weight = served[None, :, ff:]

    pre = jnp.dot(
        rows, relative(served.reshape(X, C, part, 2 * ff), ix, ic), preferred_element_type=F32
    )
    clipped = jnp.minimum(pre[:, :ff], CLAMP_LIMIT)
    hidden = (
        (jnp.clip(pre[:, ff:], -CLAMP_LIMIT, CLAMP_LIMIT) + 1.0)
        * clipped
        * jax.nn.sigmoid(SLOPE_ALPHA * clipped)
    ).astype(BF)
    near = [hidden, None, None, None]
    for k in (2, 1, 3):
        near[k] = lax.ppermute(hidden, "x", ring(X, k))
    other = [lax.ppermute(a, "c", ring(C, 1)) for a in near]
    pairs = [(near[k], other[k]) for k in range(X)]

    down_blocks = down_cols.reshape(X, C, ff, part)
    total = matched(pairs, down_blocks, ix, ic).astype(BF)
    total, down_blocks = lax.optimization_barrier((total, down_blocks))
    result = exchange(total.reshape(n_exp, CAP, part), FS)

    kept = lax.dynamic_index_in_dim(down_blocks, ic, 1, keepdims=False)
    given = lax.dynamic_index_in_dim(down_blocks, 1 - ic, 1, keepdims=False)
    taken = lax.ppermute(given, "c", ring(C, 1))
    first = jnp.where(ic == 0, kept, taken)
    second = jnp.where(ic == 0, taken, kept)
    wide_rows = jnp.concatenate([first, second], axis=2)
    cols = []
    for k in range(X):
        block = lax.dynamic_index_in_dim(wide_rows, (ix + k) % X, 0, keepdims=False)
        cols.append(block if k == 0 else lax.ppermute(block, "x", ring(X, k)))
    around = jnp.stack([cols[(-j) % X] for j in range(X)] * 2, axis=0)
    ordered = lax.dynamic_slice_in_dim(around, (X - ix) % X, X, 0)
    down_weight = ordered.transpose(1, 0, 2).reshape(1, ff, width)

    spread = jnp.where(at_slot, weight[:, None, :], 0.0).reshape(n_exp * CAP, n_tok)
    high = lax.reduce_precision(spread, 8, 7)
    contract = (((0,), (0,)), ((), ()))
    result = result.reshape(n_exp * CAP, part)
    mixed = lax.dot_general(
        high.astype(BF), result, contract, preferred_element_type=F32
    ) + lax.dot_general((spread - high).astype(BF), result, contract, preferred_element_type=F32)
    return (mixed.astype(BF), gate_weight, up_weight, down_weight)


def solution(mesh):
    fine = Mesh(mesh.devices.reshape(GR, ZL, Y, X, C), ("gr", "zl", "y", "x", "c"))
    rows, tp = ("gr", "zl", "y"), ("x", "c")
    placed = (
        P(rows, None),
        P(rows),
        P(None, rows, tp),
        P(None, rows, tp),
        P(None, rows, tp),
        P(rows, None),
        P(rows, None),
    )
    return jax.shard_map(
        layer,
        mesh=fine,
        in_specs=placed,
        out_specs=(
            P(rows, tp),
            P(FS, None, tp),
            P(FS, None, tp),
            P(FS, tp, None),
        ),
        check_vma=False,
    )
```
